32 devices in a mesh: ep: 8 (over z, y), tp: 4 (over x, core).
Axes of the slice: x: 2, y: 2, z: 4, core: 2. Of those that a mesh axis runs over, the one named last changes fastest.
Arguments:
- att_queries: bfloat16 [8192, 1024], P(('ep', 'tp')), may hold values from -8 to 8
- att_keys: bfloat16 [8192, 256], P(('ep', 'tp')), may hold values from -6 to 6
- att_values: bfloat16 [8192, 256], P(('ep', 'tp')), may hold values from -6 to 6
- sink_logits: float32 [16], replicated, may hold values from 3 to 6.5
- out_weight: bfloat16 [1024, 2048], replicated, may hold values from -0.1875 to 0.1875
- att_gain: float32 [2048], replicated, may hold values from 0.1 to 1.9
- moe_in: bfloat16 [4096, 2048], P(('ep', 'tp')), may hold values from -6 to 6
- pre_gain: float32 [2048], replicated, may hold values from 0.1 to 1.9
- expert_ids: int32 [4096, 2], P(('ep', 'tp')), may hold values from 0 to 15, all different within a row; in each aligned block of 128 rows (0 to 127, 128 to 255, ...) at most 32 rows name the same one
- routed_expert_weight: float32 [4096, 2], P(('ep', 'tp')), may hold values from 0.2 to 1.5
- w_gate: bfloat16 [16, 2048, 768], P('ep', None, 'tp'), may hold values from -0.125 to 0.125
- w_up: bfloat16 [16, 2048, 768], P('ep', None, 'tp'), may hold values from -0.125 to 0.125
- w_down: bfloat16 [16, 768, 2048], P('ep', 'tp'), may hold values from -0.21875 to 0.21875
- common_expert_gate_weight: bfloat16 [2048, 512], P(None, 'tp'), may hold values from -0.125 to 0.125
- common_expert_up_weight: bfloat16 [2048, 512], P(None, 'tp'), may hold values from -0.125 to 0.125
- common_expert_down_weight: bfloat16 [512, 2048], P('tp'), may hold values from -0.25 to 0.25
- moe_gain: float32 [2048], replicated, may hold values from 0.1 to 1.9
Outputs:
- mixer_out: bfloat16 [8192, 2048], P(('ep', 'tp'))
- experts_out: bfloat16 [4096, 2048], P(('ep', 'tp'))
The draws below stay inside these ranges and needn't reach their ends.
Inputs may be any that keep to these rules, and one draw needn't show every extreme that they name: `expert_ids`: each row names 2 different experts; within the rows of one device no expert is named more than 32 times, and in every draw some expert is named exactly 32 times by the rows of some device.
All inputs are finite; a program needn't handle non-finite values.
Results may differ from the reference program's by a relative error of at most 0.012.
Values may be sent and summed in bfloat16 or wider, within the bound.
No kernel may reach another device: no remote copies, remote signals or barrier semaphores. Data moves between devices by JAX's collectives and lax.ppermute only.
A program may use at most 128 MiB of HBM per device.

```python
import math
import jax
import jax.numpy as jnp
import numpy as np
from jax import lax

D = 2048
HEADS = 16
KV_HEADS = 4
HEAD_DIM = 64
WINDOW = 128
TOK_MOE = 128
TOPK = 2
FE = 768
SHARED = 512
EXPERTS = 16
CAP = 32
SEQ_ATT = 8192
TOKENS_MOE = 4096
N_EP = 8
N_TP = 4


def draw_att_queries(key, part):
    shape = (SEQ_ATT, KV_HEADS, HEADS // KV_HEADS, HEAD_DIM)
    base_draw = jax.random.truncated_normal(jax.random.fold_in(key, 21), -6.0, 6.0, shape, jnp.float32)
    return base_draw.reshape(SEQ_ATT, HEADS * HEAD_DIM).astype(jnp.bfloat16)


def draw_att_keys(key, part):
    shape = (SEQ_ATT, KV_HEADS, HEAD_DIM)
    base_draw = jax.random.truncated_normal(jax.random.fold_in(key, 31), -6.0, 6.0, shape, jnp.float32)
    return base_draw.reshape(SEQ_ATT, KV_HEADS * HEAD_DIM).astype(jnp.bfloat16)


def block_scale(stream_key, extent, cuts, least, largest):
    def one(dim, blocks):
        heights = jax.random.uniform(jax.random.fold_in(jax.random.fold_in(stream_key, 6), dim), (blocks,), jnp.float32, least / len(cuts), largest / len(cuts))
        return jnp.repeat(jnp.exp(heights), extent[dim] // blocks).reshape((-1,) + (1,) * (len(extent) - dim - 1))

    gain = one(*cuts[0])
    for cut in cuts[1:]:
        gain = gain * one(*cut)
    return gain


def deal_out(key, own, number, rows, amount, top, limit, lean):
    order = jax.random.permutation(key, amount)
    crowded, common = shares(amount, rows * top, limit, lean, True), shares(amount, rows * top, limit, lean, False)
    places = jnp.arange(amount)

    def named(tallies, rotation):
        used = int((tallies > 0).sum())
        fixed = max(1, used // 4)
        shifted = fixed + (places - fixed + rotation * (used - fixed)) % max(1, amount - fixed)
        return jnp.zeros((amount,), jnp.int32).at[order[jnp.where(places < fixed, places, shifted)]].set(jnp.asarray(tallies, jnp.int32))

    tallies = jnp.where(number % 4 == 0, named(crowded, number // 4), named(common, number - number // 4 - 1))
    mixed = jax.random.permutation(jax.random.fold_in(own, 3), amount)
    giver, taker = mixed[0:amount // 2 * 2:2], mixed[1:amount // 2 * 2:2]
    slack = jnp.minimum(tallies[giver] - 1, limit - tallies[taker]) // 2
    slack = jnp.where((giver == order[0]) | (taker == order[0]) | (tallies[taker] == 0), 0, jnp.maximum(slack, 0))
    shifted = jax.random.randint(jax.random.fold_in(own, 4), (amount // 2,), 0, 1 << 20) % (slack + 1)
    tallies = tallies.at[giver].add(-shifted).at[taker].add(shifted)
    members = jnp.searchsorted(jnp.cumsum(tallies), jnp.arange(rows * top), side="right").astype(jnp.int32)
    table = members.reshape(top, rows).T
    table = table[jax.random.permutation(jax.random.fold_in(own, 1), rows)]
    rotation = jax.random.randint(jax.random.fold_in(own, 2), (rows, 1), 0, top)
    return jnp.take_along_axis(table, (jnp.arange(top)[None, :] + rotation) % top, axis=1)


def shares(count, total, reach, lean, full):
    portions = [(1 << 20) // math.isqrt(rank ** lean) + 1 for rank in range(1, count + 1)]
    largest = reach if full else min(reach, max(-(-total // count), total * portions[0] // sum(portions)))
    least = 1 if total - largest >= count - 1 else 0
    given, rest = [largest] + [least] * (count - 1), total - largest - least * (count - 1)
    while rest > 0:
        free = [i for i in range(1, count) if given[i] < largest] or [i for i in range(1, count) if given[i] < reach]
        whole, budget = sum([portions[i] for i in free]), rest
        for i in free:
            more = min(reach - given[i], max(1, budget * portions[i] // whole), rest)
            given[i] = given[i] + more
            rest = rest - more
    return np.array(given)


def centred(stream_key, dims, width, reach, shards=(), kind=jnp.bfloat16):
    values = width * jax.random.normal(stream_key, dims, jnp.float32)
    if shards:
        values = values * block_scale(stream_key, dims, shards, -0.22, 0.18)
    return jnp.clip(values, -reach, reach).astype(kind)


def setup_inputs(seed: int = 0) -> dict:
    key_list = jax.random.split(jax.random.key(seed), 18)
    att_queries = draw_att_queries(jax.random.fold_in(key_list[17], 71), 0)
    att_keys = draw_att_keys(jax.random.fold_in(key_list[17], 71), 0)
    att_values = centred(key_list[2], (SEQ_ATT, KV_HEADS * HEAD_DIM), 1.0, 6.0, ((0, 32),))
    sink_logits = jnp.clip(jax.random.uniform(key_list[3], (HEADS,), jnp.float32, 3.0, 6.5), 3.0, 6.5)
    out_weight = centred(key_list[4], (HEADS * HEAD_DIM, D), (HEADS * HEAD_DIM) ** -0.5, 0.1875)
    att_gain = jnp.clip(1.0 + 0.18 * jax.random.normal(key_list[5], (D,), jnp.float32), 0.1, 1.9)
    moe_in = centred(key_list[6], (TOKENS_MOE, D), 1.0, 6.0, ((0, 32),))
    pre_gain = jnp.clip(1.0 + 0.18 * jax.random.normal(key_list[7], (D,), jnp.float32), 0.1, 1.9)
    expert_ids_keys = jax.random.split(jax.random.fold_in(key_list[8], 1), TOKENS_MOE // TOK_MOE)
    expert_ids_turns = jax.random.permutation(jax.random.fold_in(key_list[8], 3), TOKENS_MOE // TOK_MOE)
    expert_ids = jax.vmap(lambda own, number: deal_out(jax.random.fold_in(key_list[8], 2), own, number, TOK_MOE, EXPERTS, TOPK, CAP, 1))(expert_ids_keys, expert_ids_turns).reshape((TOKENS_MOE, TOPK))
    routed_expert_weight = jnp.clip(jnp.exp(math.log(1.5) - 2.014903 * jax.random.uniform(key_list[9], (TOKENS_MOE, TOPK), jnp.float32) ** block_scale(key_list[9], (TOKENS_MOE, TOPK), ((0, 32),), -0.2, 0.2)), 0.2, 1.5)
    w_gate = centred(key_list[10], (EXPERTS, D, FE), D ** -0.5, 0.125, ((0, 8), (2, 4)))
    w_up = centred(key_list[11], (EXPERTS, D, FE), D ** -0.5, 0.125, ((0, 8), (2, 4)))
    w_down = centred(key_list[12], (EXPERTS, FE, D), FE ** -0.5, 0.21875, ((0, 8), (1, 4)))
    common_expert_gate_weight = centred(key_list[13], (D, SHARED), D ** -0.5, 0.125, ((1, 4),))
    common_expert_up_weight = centred(key_list[14], (D, SHARED), D ** -0.5, 0.125, ((1, 4),))
    common_expert_down_weight = centred(key_list[15], (SHARED, D), SHARED ** -0.5, 0.25, ((0, 4),))
    moe_gain = jnp.clip(1.0 + 0.18 * jax.random.normal(key_list[16], (D,), jnp.float32), 0.1, 1.9)
    return {"att_queries": att_queries, "att_keys": att_keys, "att_values": att_values, "sink_logits": sink_logits, "out_weight": out_weight, "att_gain": att_gain, "moe_in": moe_in, "pre_gain": pre_gain, "expert_ids": expert_ids, "routed_expert_weight": routed_expert_weight, "w_gate": w_gate, "w_up": w_up, "w_down": w_down, "common_expert_gate_weight": common_expert_gate_weight, "common_expert_up_weight": common_expert_up_weight, "common_expert_down_weight": common_expert_down_weight, "moe_gain": moe_gain}


EPS = 1e-06
NEGATIVE = -1e+30

def rms_scale(inputs, gain_vec):
    mean_sq = lax.optimization_barrier(jnp.mean(inputs * inputs, axis=-1, keepdims=True))
    return inputs * lax.rsqrt(mean_sq + EPS) * gain_vec

def block_parts(hidden, down_rows, split_count):
    block_width = hidden.shape[-1] // split_count
    pieces = jnp.einsum('rbf,bfd->rbd', hidden.astype(jnp.float32).reshape(hidden.shape[0], split_count, block_width), down_rows.astype(jnp.float32).reshape(split_count, block_width, down_rows.shape[-1]))
    rounded = lax.optimization_barrier(pieces.astype(jnp.bfloat16))
    return lax.optimization_barrier(jnp.sum(rounded.astype(jnp.float32), axis=1))

def window_attention(att_queries, att_keys, att_values, sink_logits):
    group_size = HEADS // KV_HEADS
    blocks = SEQ_ATT // WINDOW
    padding = jnp.zeros((WINDOW, KV_HEADS * HEAD_DIM), att_keys.dtype)
    key_blocks = jnp.concatenate([padding, att_keys], axis=0).reshape(blocks + 1, WINDOW, KV_HEADS, HEAD_DIM)
    value_blocks = jnp.concatenate([padding, att_values], axis=0).reshape(blocks + 1, WINDOW, KV_HEADS, HEAD_DIM)
    query_blocks = att_queries.reshape(blocks, WINDOW, KV_HEADS, group_size, HEAD_DIM)
    distance = jnp.arange(WINDOW)[:, None] + WINDOW - jnp.arange(2 * WINDOW)[None, :]
    inside = (distance >= 0) & (distance < WINDOW)
    sink_grid = sink_logits.astype(jnp.float32).reshape(KV_HEADS, group_size)[:, :, None, None]
    score_scale = 1.0 / math.sqrt(HEAD_DIM)

    def one_block(block_index):
        key_band = lax.dynamic_slice_in_dim(key_blocks, block_index, 2, 0).reshape(2 * WINDOW, KV_HEADS, HEAD_DIM)
        value_band = lax.dynamic_slice_in_dim(value_blocks, block_index, 2, 0).reshape(2 * WINDOW, KV_HEADS, HEAD_DIM)
        query_block = lax.dynamic_index_in_dim(query_blocks, block_index, 0, keepdims=False)
        scores = jnp.einsum('qgjd,kgd->gjqk', query_block.astype(jnp.float32), key_band.astype(jnp.float32)) * score_scale
        key_pos = block_index * WINDOW - WINDOW + jnp.arange(2 * WINDOW)
        is_valid = inside & (key_pos >= 0)[None, :]
        scores = jnp.where(is_valid[None, None], scores, NEGATIVE)
        row_top = jnp.maximum(lax.optimization_barrier(jnp.max(scores, axis=-1, keepdims=True)), sink_grid)
        exp_scores = jnp.exp(scores - row_top)
        denominator = lax.optimization_barrier(jnp.sum(exp_scores, axis=-1, keepdims=True)) + jnp.exp(sink_grid - row_top)
        probs = (exp_scores / denominator).astype(jnp.bfloat16)
        head_mix = jnp.einsum('gjqk,kgd->qgjd', probs.astype(jnp.float32), value_band.astype(jnp.float32))
        return head_mix.astype(jnp.bfloat16).reshape(WINDOW, HEADS * HEAD_DIM)
    head_mix = lax.map(one_block, jnp.arange(blocks, dtype=jnp.int32))
    return head_mix.reshape(SEQ_ATT, HEADS * HEAD_DIM)

def routed_experts(normed, expert_ids, routed_expert_weight, w_gate, w_up, w_down):
    devices = N_EP * N_TP
    per_device = TOK_MOE * TOPK
    flat_ids = expert_ids.reshape(devices, per_device)
    earlier = jnp.arange(per_device)[None, :] < jnp.arange(per_device)[:, None]

    def positions_of(device_ids):
        return lax.optimization_barrier(jnp.sum((device_ids[:, None] == device_ids[None, :]) & earlier, axis=1)).astype(jnp.int32)
    position = lax.map(positions_of, flat_ids)
    device_index = jnp.arange(devices, dtype=jnp.int32)[:, None]
    slot_index = ((flat_ids * devices + device_index) * CAP + position).reshape(-1).astype(jnp.int32)
    token_index = (device_index * TOK_MOE + jnp.arange(per_device, dtype=jnp.int32)[None, :] // TOPK).reshape(-1)
    table_size = EXPERTS * devices * CAP
    row_table = jnp.zeros((table_size,), jnp.int32).at[slot_index].set(token_index.astype(jnp.int32))
    row_table = row_table.reshape(EXPERTS, devices * CAP)
    weight_table = jnp.zeros((table_size,), jnp.float32).at[slot_index].set(routed_expert_weight.reshape(-1))
    weight_table = weight_table.reshape(EXPERTS, devices * CAP)

    def add_expert(running, expert_index):
        row_ids = lax.dynamic_index_in_dim(row_table, expert_index, 0, keepdims=False)
        slot_weights = lax.dynamic_index_in_dim(weight_table, expert_index, 0, keepdims=False)
        picked = normed[row_ids]
        gate_act = jnp.dot(picked, w_gate[expert_index], preferred_element_type=jnp.float32)
        up_act = jnp.dot(picked, w_up[expert_index], preferred_element_type=jnp.float32)
        hidden = (jax.nn.silu(gate_act) * up_act).astype(jnp.bfloat16)
        output = block_parts(hidden, w_down[expert_index], N_TP).astype(jnp.bfloat16)
        running = running.at[row_ids].add(slot_weights[:, None] * output.astype(jnp.float32))
        return (running, None)
    start_value = jnp.zeros((TOKENS_MOE, D), jnp.float32)
    return lax.scan(add_expert, start_value, jnp.arange(EXPERTS, dtype=jnp.int32))[0]

def reference(att_queries, att_keys, att_values, sink_logits, out_weight, att_gain, moe_in, pre_gain, expert_ids, routed_expert_weight, w_gate, w_up, w_down, common_expert_gate_weight, common_expert_up_weight, common_expert_down_weight, moe_gain):
    head_mix = window_attention(att_queries, att_keys, att_values, sink_logits)
    projected = jnp.dot(head_mix, out_weight, preferred_element_type=jnp.float32)
    mixer_out = rms_scale(projected, att_gain).astype(jnp.bfloat16)
    normed = rms_scale(moe_in.astype(jnp.float32), pre_gain).astype(jnp.bfloat16)
    routed = routed_experts(normed, expert_ids, routed_expert_weight, w_gate, w_up, w_down)

    def shared_rows(row_block):
        gate_act = jnp.dot(row_block, common_expert_gate_weight, preferred_element_type=jnp.float32)
        up_act = jnp.dot(row_block, common_expert_up_weight, preferred_element_type=jnp.float32)
        common_expert_hidden = (jax.nn.silu(gate_act) * up_act).astype(jnp.bfloat16)
        return block_parts(common_expert_hidden, common_expert_down_weight, N_TP)
    shared_sum = lax.map(shared_rows, normed.reshape(N_EP * N_TP, TOK_MOE, D)).reshape(TOKENS_MOE, D)
    combined = routed + shared_sum
    experts_out = rms_scale(combined, moe_gain).astype(jnp.bfloat16)
    return (mixer_out, experts_out)
```

```python
import math

import jax
import jax.numpy as jnp
from jax import lax
from jax.sharding import PartitionSpec as P

HEADS = 16
KV_HEADS = 4
HEAD_DIM = 64
WINDOW = 128


EPS = 1e-06
NEGATIVE = -1e30
NEAR_LIMIT = 8


def from_behind(block, axis, distance):
    devices = range(lax.axis_size(axis))
    route = [(i - distance, i) for i in devices if i - distance in devices]
    return lax.ppermute(block, axis, route)


def rms_scale(inputs, gain_vec):
    mean_sq = jnp.mean(inputs * inputs, axis=-1, keepdims=True)
    return inputs * lax.rsqrt(mean_sq + EPS) * gain_vec


def slot_table(route_ids, slot_cap):
    flat_ids = route_ids.reshape(-1)
    assigned = flat_ids.shape[0]
    earlier = jnp.arange(assigned)[None, :] < jnp.arange(assigned)[:, None]
    position = jnp.sum((flat_ids[:, None] == flat_ids[None, :]) & earlier, axis=1)
    return (flat_ids * slot_cap + position).reshape(route_ids.shape)


def pack_rows(token_rows, slot_ids, slot_total):
    numbers = jnp.arange(slot_total, dtype=jnp.int32)
    chosen = jnp.any(slot_ids[None, :, :] == numbers[:, None, None], axis=2).astype(jnp.bfloat16)
    return jnp.dot(chosen, token_rows, preferred_element_type=jnp.float32).astype(jnp.bfloat16)


def attention(
    att_queries,
    att_keys,
    att_values,
    sink_logits,
    out_weight,
    att_gain,
):
    tok_rows = att_queries.shape[0]
    group_size = HEADS // KV_HEADS
    blocks = tok_rows // WINDOW
    kv_rows = jnp.stack([att_keys, att_values])
    rim_rows = from_behind(kv_rows[:, tok_rows - WINDOW :], ("ep", "tp"), 1)
    kv_all = jnp.concatenate([rim_rows, kv_rows], axis=1).reshape(
        2, blocks + 1, WINDOW, KV_HEADS, HEAD_DIM
    )
    kv_band = jnp.concatenate([kv_all[:, :-1], kv_all[:, 1:]], axis=2)
    query_blocks = att_queries.reshape(blocks, WINDOW, KV_HEADS, group_size, HEAD_DIM)
    scores = jnp.einsum(
        "nqgjd,nkgd->ngjqk", query_blocks, kv_band[0], preferred_element_type=jnp.float32
    ) * (1.0 / math.sqrt(HEAD_DIM))
    distance = jnp.arange(WINDOW)[:, None] + WINDOW - jnp.arange(2 * WINDOW)[None, :]
    inside = (distance >= 0) & (distance < WINDOW)
    first_pos = lax.axis_index(("ep", "tp")) * tok_rows
    key_pos = (
        first_pos + jnp.arange(blocks)[:, None] * WINDOW - WINDOW + jnp.arange(2 * WINDOW)[None, :]
    )
    is_valid = inside[None] & (key_pos >= 0)[:, None, :]
    scores = jnp.where(is_valid[:, None, None], scores, NEGATIVE)
    sink_grid = sink_logits.reshape(KV_HEADS, group_size)[None, :, :, None, None]
    row_top = jnp.maximum(jnp.max(scores, axis=-1, keepdims=True), sink_grid)
    exp_scores = jnp.exp(scores - row_top)
    denominator = jnp.sum(exp_scores, axis=-1, keepdims=True) + jnp.exp(sink_grid - row_top)
    probs = (exp_scores / denominator).astype(jnp.bfloat16)
    head_mix = jnp.einsum(
        "ngjqk,nkgd->nqgjd", probs, kv_band[1], preferred_element_type=jnp.float32
    )
    head_mix = head_mix.astype(jnp.bfloat16).reshape(tok_rows, HEADS * HEAD_DIM)
    projected = jnp.dot(head_mix, out_weight, preferred_element_type=jnp.float32)
    return rms_scale(projected, att_gain).astype(jnp.bfloat16)


def experts_wide(
    moe_in,
    pre_gain,
    expert_ids,
    routed_expert_weight,
    w_gate,
    w_up,
    w_down,
    common_expert_gate_weight,
    common_expert_up_weight,
    common_expert_down_weight,
    moe_gain,
):
    tokens = moe_in.shape[0]
    top_count = expert_ids.shape[1]
    local_experts = w_gate.shape[0]
    ep_size = lax.axis_size("ep")
    tp_size = lax.axis_size("tp")
    experts = local_experts * ep_size
    slot_cap = 2 * tokens * top_count // experts
    slot_total = experts * slot_cap
    normed = rms_scale(moe_in.astype(jnp.float32), pre_gain).astype(jnp.bfloat16)
    own_slots = slot_table(expert_ids, slot_cap)
    packed = pack_rows(normed, own_slots, slot_total)[None]
    arrived = lax.all_to_all(packed, "ep", split_axis=1, concat_axis=1, tiled=True)
    arrived_all, tokens_all = (
        lax.all_gather(arrived[0], "tp", axis=0, tiled=True),
        lax.all_gather(normed, "tp", axis=0, tiled=True),
    )
    arrived = arrived_all.reshape(tp_size, slot_total, normed.shape[1])
    token_block = tokens_all.reshape(tp_size, tokens, normed.shape[1])
    routed = arrived
    routed = routed.reshape(
        1 * lax.axis_size("tp"), ep_size, local_experts, slot_cap, normed.shape[1]
    )
    gate_act = jnp.einsum("tsjcd,jdf->tsjcf", routed, w_gate, preferred_element_type=jnp.float32)
    up_act = jnp.einsum("tsjcd,jdf->tsjcf", routed, w_up, preferred_element_type=jnp.float32)
    hidden = (jax.nn.silu(gate_act) * up_act).astype(jnp.bfloat16)
    routed_part = jnp.einsum("tsjcf,jfd->tsjcd", hidden, w_down, preferred_element_type=jnp.float32)
    routed_part = routed_part.reshape(1 * lax.axis_size("tp"), slot_total, normed.shape[1])
    common_gate_activation = jnp.einsum(
        "spz,zv->spv", token_block, common_expert_gate_weight, preferred_element_type=jnp.float32
    )
    shared_up_act = jnp.einsum(
        "spz,zv->spv", token_block, common_expert_up_weight, preferred_element_type=jnp.float32
    )
    common_expert_hidden = (jax.nn.silu(common_gate_activation) * shared_up_act).astype(
        jnp.bfloat16
    )
    shared_part = jnp.einsum(
        "nsq,ql->nsl",
        common_expert_hidden,
        common_expert_down_weight,
        preferred_element_type=jnp.float32,
    )
    summed = lax.psum_scatter(
        jnp.concatenate([routed_part, shared_part], axis=1).astype(jnp.bfloat16),
        "tp",
        scatter_dimension=0,
        tiled=True,
    ).astype(jnp.float32)
    routed_out = summed[0, :slot_total].astype(jnp.bfloat16)
    shared_sum = summed[0, slot_total:]
    returned = lax.all_to_all(routed_out, "ep", split_axis=0, concat_axis=0, tiled=True)
    picked = returned[own_slots.reshape(-1)].reshape(tokens, top_count, normed.shape[1])
    combined = (
        jnp.sum(routed_expert_weight[:, :, None] * picked.astype(jnp.float32), axis=1) + shared_sum
    )
    experts_out = rms_scale(combined, moe_gain).astype(jnp.bfloat16)
    return experts_out


def swap(block, axis, bit):
    route = [(i, i ^ bit) for i in range(lax.axis_size(axis))]
    return lax.ppermute(block, axis, route)


def glu(rows, gate, up, down):
    gate_act = jnp.einsum("jcd,jdf->jcf", rows, gate, preferred_element_type=jnp.float32)
    up_act = jnp.einsum("jcd,jdf->jcf", rows, up, preferred_element_type=jnp.float32)
    hidden = (jax.nn.silu(gate_act) * up_act).astype(jnp.bfloat16)
    return jnp.einsum("jcf,jfd->jcd", hidden, down, preferred_element_type=jnp.float32)


def experts_near(
    moe_in,
    pre_gain,
    expert_ids,
    routed_expert_weight,
    w_gate,
    w_up,
    w_down,
    common_expert_gate_weight,
    common_expert_up_weight,
    common_expert_down_weight,
    moe_gain,
):
    tokens, width = moe_in.shape
    top_count = expert_ids.shape[1]
    local_experts = w_gate.shape[0]
    ep_size = lax.axis_size("ep")
    near_bit, far_bit = 1, lax.axis_size("tp") // 2
    experts = local_experts * ep_size
    slot_cap = 2 * tokens * top_count // experts
    slot_total = experts * slot_cap
    own = lax.axis_index("ep")

    def paired(block, axis):
        return jnp.concatenate([block, swap(block, "tp", near_bit)], axis=axis)

    gate, up, down = paired(w_gate, 2), paired(w_up, 2), paired(w_down, 1)
    shared_gate = paired(common_expert_gate_weight, 1)[None]
    shared_up = paired(common_expert_up_weight, 1)[None]
    shared_down = paired(common_expert_down_weight, 0)[None]

    normed = rms_scale(moe_in.astype(jnp.float32), pre_gain).astype(jnp.bfloat16)
    relative = ((expert_ids // local_experts) ^ own) * local_experts + expert_ids % local_experts
    own_slots = slot_table(relative, slot_cap)
    numbers = jnp.arange(slot_total, dtype=jnp.int32)
    hits = own_slots[:, :, None] == numbers[None, None, :]
    share = jnp.sum(jnp.where(hits, routed_expert_weight[:, :, None], 0.0), axis=1)
    share_top = share.astype(jnp.bfloat16)
    share_rest = (share - share_top.astype(jnp.float32)).astype(jnp.bfloat16)
    packed = pack_rows(normed, own_slots, slot_total)
    packed = packed.reshape(ep_size, local_experts, slot_cap, width)

    token_rows = jnp.stack([normed, swap(normed, "tp", far_bit)]).reshape(1, 2 * tokens, width)
    arrived = [packed[0]] + [swap(packed[r], "ep", r) for r in range(1, ep_size)]
    shared = glu(token_rows, shared_gate, shared_up, shared_down)[0]
    shared_sum = shared[:tokens] + swap(shared[tokens:].astype(jnp.bfloat16), "tp", far_bit)

    combined = shared_sum
    step = 2
    for first in range(0, ep_size, step):
        rows = jnp.concatenate(arrived[first : first + step], axis=1)
        both = jnp.concatenate([rows, swap(rows, "tp", far_bit)], axis=1)
        part = glu(both, gate, up, down).astype(jnp.bfloat16)
        half = rows.shape[1]
        back = swap(part[:, half:], "tp", far_bit)
        total = (part[:, :half].astype(jnp.float32) + back.astype(jnp.float32)).astype(jnp.bfloat16)
        for r in range(first, first + step):
            piece = total[:, (r - first) * slot_cap : (r - first + 1) * slot_cap]
            if r:
                piece = swap(piece, "ep", r)
            piece = piece.reshape(local_experts * slot_cap, width)
            at = slice(r * local_experts * slot_cap, (r + 1) * local_experts * slot_cap)
            for table in (share_top, share_rest):
                combined = combined + jnp.dot(
                    table[:, at], piece, preferred_element_type=jnp.float32
                )
    return rms_scale(combined, moe_gain).astype(jnp.bfloat16)


def body(*args):
    mixer_out = attention(*args[:6])
    ep_size = lax.axis_size("ep")
    near = ep_size <= NEAR_LIMIT and ep_size & (ep_size - 1) == 0 and lax.axis_size("tp") == 4
    experts_out = (experts_near if near else experts_wide)(*args[6:])
    return (mixer_out, experts_out)


def solution(mesh):
    in_specs = (
        P(("ep", "tp"), None),
        P(("ep", "tp"), None),
        P(("ep", "tp"), None),
        P(),
        P(),
        P(),
        P(("ep", "tp"), None),
        P(),
        P(("ep", "tp"), None),
        P(("ep", "tp"), None),
        P("ep", None, "tp"),
        P("ep", None, "tp"),
        P("ep", "tp", None),
        P(None, "tp"),
        P(None, "tp"),
        P("tp", None),
        P(),
    )
    out_specs = (P(("ep", "tp"), None), P(("ep", "tp"), None))
    return jax.shard_map(body, mesh=mesh, in_specs=in_specs, out_specs=out_specs, check_vma=False)
```

```python
import functools
import math

import jax
import jax.numpy as jnp
from jax import lax
from jax.experimental import pallas as pl
from jax.experimental.pallas import tpu as pltpu
from jax.sharding import PartitionSpec as P

HEADS = 16
KV_HEADS = 4
HEAD_DIM = 64
WINDOW = 128


EPS = 1e-06
NEGATIVE = -1e30
NEAR_LIMIT = 8
KERNEL_VMEM = 24 * 1024 * 1024


def from_behind(block, axis, distance):
    devices = range(lax.axis_size(axis))
    route = [(i - distance, i) for i in devices if i - distance in devices]
    return lax.ppermute(block, axis, route)


def rms_scale(inputs, gain_vec):
    mean_sq = jnp.mean(inputs * inputs, axis=-1, keepdims=True)
    return inputs * lax.rsqrt(mean_sq + EPS) * gain_vec


def slot_table(route_ids, slot_cap):
    flat_ids = route_ids.reshape(-1)
    assigned = flat_ids.shape[0]
    earlier = jnp.arange(assigned)[None, :] < jnp.arange(assigned)[:, None]
    position = jnp.sum((flat_ids[:, None] == flat_ids[None, :]) & earlier, axis=1)
    return (flat_ids * slot_cap + position).reshape(route_ids.shape)


def pack_rows(token_rows, slot_ids, slot_total):
    numbers = jnp.arange(slot_total, dtype=jnp.int32)
    chosen = jnp.any(slot_ids[None, :, :] == numbers[:, None, None], axis=2).astype(jnp.bfloat16)
    return jnp.dot(chosen, token_rows, preferred_element_type=jnp.float32).astype(jnp.bfloat16)


def attention_kernel(q_ref, k_ref, v_ref, rim_ref, sink_ref, first_ref, weight_ref, gain_ref, out_ref, mix_ref):
    lanes = 2 * HEAD_DIM
    group_size = HEADS // KV_HEADS
    blocks = q_ref.shape[0] // WINDOW
    query = lax.broadcasted_iota(jnp.int32, (WINDOW, 2 * WINDOW), 0)
    key = lax.broadcasted_iota(jnp.int32, (WINDOW, 2 * WINDOW), 1)
    inside = (key > query) & (key <= query + WINDOW)
    low = lax.broadcasted_iota(jnp.int32, (2 * WINDOW, lanes), 1) < HEAD_DIM

    def spread(tile, group):
        tile = tile.astype(jnp.float32)
        kept = jnp.where(low if group % 2 == 0 else ~low, tile, 0.0)
        moved = pltpu.roll(kept, HEAD_DIM, 1)
        both = [kept, moved] if group % 2 == 0 else [moved, kept]
        return jnp.concatenate(both, axis=0).astype(jnp.bfloat16)

    for block in range(blocks):
        at = slice(block * WINDOW, (block + 1) * WINDOW)
        before = slice((block - 1) * WINDOW, block * WINDOW)
        valid = inside
        if block == 0:
            valid = inside & (key >= first_ref[0] * WINDOW)
        for tile in range(KV_HEADS // 2):
            span = slice(tile * lanes, (tile + 1) * lanes)
            earlier_k = rim_ref[0, :, span] if block == 0 else k_ref[before, span]
            earlier_v = rim_ref[1, :, span] if block == 0 else v_ref[before, span]
            band_k = jnp.concatenate([earlier_k, k_ref[at, span]], axis=0)
            band_v = jnp.concatenate([earlier_v, v_ref[at, span]], axis=0)
            for group in (2 * tile, 2 * tile + 1):
                keys, values = spread(band_k, group), spread(band_v, group)
                for pair in range(group * group_size // 2, (group + 1) * group_size // 2):
                    cols = slice(pair * lanes, (pair + 1) * lanes)
                    scores = dot_last(q_ref[at, cols], keys) * (1.0 / math.sqrt(HEAD_DIM))
                    probs = []
                    for part in range(2):
                        sink = sink_ref[2 * pair + part]
                        own = scores[:, part * 2 * WINDOW : (part + 1) * 2 * WINDOW]
                        own = jnp.where(valid, own, NEGATIVE)
                        row_top = jnp.maximum(jnp.max(own, axis=-1, keepdims=True), sink)
                        grown = jnp.exp(own - row_top)
                        total = jnp.sum(grown, axis=-1, keepdims=True) + jnp.exp(sink - row_top)
                        probs.append((grown * (1.0 / total)).astype(jnp.bfloat16))
                    mixed = jnp.dot(
                        jnp.concatenate(probs, axis=1), values, preferred_element_type=jnp.float32
                    )
                    mix_ref[at, cols] = mixed.astype(jnp.bfloat16)
    projected = jnp.dot(mix_ref[...], weight_ref[...], preferred_element_type=jnp.float32)
    mean_sq = jnp.mean(projected * projected, axis=-1, keepdims=True)
    out_ref[...] = (projected * lax.rsqrt(mean_sq + EPS) * gain_ref[...]).astype(jnp.bfloat16)


def attention(att_queries, att_keys, att_values, sink_logits, out_weight, att_gain):
    rows, columns = att_queries.shape
    width = out_weight.shape[1]
    last = slice(rows - WINDOW, rows)
    rim = from_behind(jnp.stack([att_keys[last], att_values[last]]), ("ep", "tp"), 1)
    first = (lax.axis_index(("ep", "tp")) == 0).astype(jnp.int32)[None]
    inner, scalars = pl.BlockSpec(memory_space=pltpu.VMEM), pl.BlockSpec(memory_space=pltpu.SMEM)
    return pl.pallas_call(
        attention_kernel,
        out_shape=jax.ShapeDtypeStruct((rows, width), jnp.bfloat16),
        in_specs=[inner] * 4 + [scalars] * 2 + [inner] * 2,
        out_specs=inner,
        scratch_shapes=[pltpu.VMEM((rows, columns), jnp.bfloat16)],
        compiler_params=pltpu.CompilerParams(vmem_limit_bytes=KERNEL_VMEM),
        cost_estimate=pl.CostEstimate(
            flops=2 * rows * columns * (width + 8 * WINDOW),
            bytes_accessed=2 * (rows * columns + columns * width + rows * width),
            transcendentals=rows * HEADS * 2 * WINDOW,
        ),
    )(att_queries, att_keys, att_values, rim, sink_logits, first, out_weight, att_gain[None])


def experts_wide(
    moe_in,
    pre_gain,
    expert_ids,
    routed_expert_weight,
    w_gate,
    w_up,
    w_down,
    common_expert_gate_weight,
    common_expert_up_weight,
    common_expert_down_weight,
    moe_gain,
):
    tokens = moe_in.shape[0]
    top_count = expert_ids.shape[1]
    local_experts = w_gate.shape[0]
    ep_size = lax.axis_size("ep")
    tp_size = lax.axis_size("tp")
    experts = local_experts * ep_size
    slot_cap = 2 * tokens * top_count // experts
    slot_total = experts * slot_cap
    normed = rms_scale(moe_in.astype(jnp.float32), pre_gain).astype(jnp.bfloat16)
    own_slots = slot_table(expert_ids, slot_cap)
    packed = pack_rows(normed, own_slots, slot_total)[None]
    arrived = lax.all_to_all(packed, "ep", split_axis=1, concat_axis=1, tiled=True)
    arrived_all, tokens_all = (
        lax.all_gather(arrived[0], "tp", axis=0, tiled=True),
        lax.all_gather(normed, "tp", axis=0, tiled=True),
    )
    arrived = arrived_all.reshape(tp_size, slot_total, normed.shape[1])
    token_block = tokens_all.reshape(tp_size, tokens, normed.shape[1])
    routed = arrived
    routed = routed.reshape(
        1 * lax.axis_size("tp"), ep_size, local_experts, slot_cap, normed.shape[1]
    )
    gate_act = jnp.einsum("tsjcd,jdf->tsjcf", routed, w_gate, preferred_element_type=jnp.float32)
    up_act = jnp.einsum("tsjcd,jdf->tsjcf", routed, w_up, preferred_element_type=jnp.float32)
    hidden = (jax.nn.silu(gate_act) * up_act).astype(jnp.bfloat16)
    routed_part = jnp.einsum("tsjcf,jfd->tsjcd", hidden, w_down, preferred_element_type=jnp.float32)
    routed_part = routed_part.reshape(1 * lax.axis_size("tp"), slot_total, normed.shape[1])
    common_gate_activation = jnp.einsum(
        "spz,zv->spv", token_block, common_expert_gate_weight, preferred_element_type=jnp.float32
    )
    shared_up_act = jnp.einsum(
        "spz,zv->spv", token_block, common_expert_up_weight, preferred_element_type=jnp.float32
    )
    common_expert_hidden = (jax.nn.silu(common_gate_activation) * shared_up_act).astype(
        jnp.bfloat16
    )
    shared_part = jnp.einsum(
        "nsq,ql->nsl",
        common_expert_hidden,
        common_expert_down_weight,
        preferred_element_type=jnp.float32,
    )
    summed = lax.psum_scatter(
        jnp.concatenate([routed_part, shared_part], axis=1).astype(jnp.bfloat16),
        "tp",
        scatter_dimension=0,
        tiled=True,
    ).astype(jnp.float32)
    routed_out = summed[0, :slot_total].astype(jnp.bfloat16)
    shared_sum = summed[0, slot_total:]
    returned = lax.all_to_all(routed_out, "ep", split_axis=0, concat_axis=0, tiled=True)
    picked = returned[own_slots.reshape(-1)].reshape(tokens, top_count, normed.shape[1])
    combined = (
        jnp.sum(routed_expert_weight[:, :, None] * picked.astype(jnp.float32), axis=1) + shared_sum
    )
    experts_out = rms_scale(combined, moe_gain).astype(jnp.bfloat16)
    return experts_out


def swap(block, axis, bit):
    route = [(i, i ^ bit) for i in range(lax.axis_size(axis))]
    return lax.ppermute(block, axis, route)


def dot_last(left, right):
    return lax.dot_general(
        left, right, (((1,), (1,)), ((), ())), preferred_element_type=jnp.float32
    )


def gated(gate_act, up_act):
    return (gate_act / (1.0 + jnp.exp(-gate_act)) * up_act).astype(jnp.bfloat16)


def run_kernel(kernel, outs, flops, *operands):
    size = sum(o.size * o.dtype.itemsize for o in (*operands, *outs))
    return pl.pallas_call(
        kernel,
        out_shape=outs,
        compiler_params=pltpu.CompilerParams(vmem_limit_bytes=KERNEL_VMEM),
        cost_estimate=pl.CostEstimate(flops=flops, bytes_accessed=size, transcendentals=0),
    )(*operands)


def prepare_kernel(cap, in_ref, gain_ref, rel_ref, weight_ref, normed_ref, top_ref, rest_ref, near_ref, *pieces):
    rows = in_ref[...].astype(jnp.float32)
    mean_sq = jnp.mean(rows * rows, axis=-1, keepdims=True)
    normed = (rows * lax.rsqrt(mean_sq + EPS) * gain_ref[...]).astype(jnp.bfloat16)
    normed_ref[...] = normed
    top_count, tokens = rel_ref.shape
    piece_rows = pieces[0].shape[0]
    slots = (1 + len(pieces)) * piece_rows
    experts = slots // cap
    expert_row = lax.broadcasted_iota(jnp.int32, (experts, tokens), 0)
    named = [rel_ref[k : k + 1, :] == expert_row for k in range(top_count)]
    counts = sum(jnp.where(hit, 1.0, 0.0) for hit in named)
    before = lax.broadcasted_iota(jnp.int32, (tokens, tokens), 0) < lax.broadcasted_iota(
        jnp.int32, (tokens, tokens), 1
    )
    prior = jnp.dot(
        counts.astype(jnp.bfloat16),
        jnp.where(before, 1.0, 0.0).astype(jnp.bfloat16),
        preferred_element_type=jnp.float32,
    )
    slot_row = lax.broadcasted_iota(jnp.int32, (slots, tokens), 0)
    chosen = jnp.zeros((slots, tokens), jnp.float32)
    share = jnp.zeros((slots, tokens), jnp.float32)
    for k, hit in enumerate(named):
        position = jnp.sum(jnp.where(hit, prior, 0.0), axis=0, keepdims=True)
        slot = rel_ref[k : k + 1, :] * cap + position.astype(jnp.int32)
        here = slot == slot_row
        chosen = chosen + jnp.where(here, 1.0, 0.0)
        share = share + jnp.where(here, weight_ref[k : k + 1, :], 0.0)
    chosen = chosen.astype(jnp.bfloat16)
    for p, piece in enumerate(pieces, 1):
        piece[...] = jnp.dot(
            chosen[p * piece_rows : (p + 1) * piece_rows],
            normed,
            preferred_element_type=jnp.float32,
        ).astype(jnp.bfloat16)
    top = share.astype(jnp.bfloat16)
    rest = (share - top.astype(jnp.float32)).astype(jnp.bfloat16)
    top_ref[...] = top[piece_rows:]
    rest_ref[...] = rest[piece_rows:]
    near_ref[...] = jnp.concatenate([t[:piece_rows] for t in (chosen, top, rest)], axis=0)


def routed(rows, j, gate_a, gate_b, up_a, up_b, down_a, down_b):
    wide = jnp.concatenate([gate_a[j], gate_b[j], up_a[j], up_b[j]], axis=0)
    act = dot_last(rows, wide)
    half = act.shape[1] // 2
    hidden = gated(act[:, :half], act[:, half:])
    down = jnp.concatenate([down_a[j], down_b[j]], axis=0)
    return jnp.dot(hidden, down, preferred_element_type=jnp.float32).astype(jnp.bfloat16)


def routed_kernel(cap, count, *refs):
    pieces, weights, outs = refs[:count], refs[count : count + 6], refs[count + 6 :]
    for j in range(weights[0].shape[0]):
        at = slice(j * cap, (j + 1) * cap)
        rows = jnp.concatenate([piece[at, :] for piece in pieces], axis=0)
        out = routed(rows, j, *weights)
        for p, out_ref in enumerate(outs):
            out_ref[at, :] = out[p * cap : (p + 1) * cap]


def local_kernel(cap, own_ref, other_ref, own_tab, other_tab, *refs):
    ga, gb, ua, ub, da, db = refs[:6]
    weights, (own_out, other_out) = refs[6:12], refs[12:]
    tokens = own_ref.shape[0]
    piece_rows = own_tab.shape[0] // 3
    rows = jnp.concatenate([own_ref[...], other_ref[...]], axis=0)
    gate = jnp.concatenate([ga[...], gb[...]], axis=1)
    up = jnp.concatenate([ua[...], ub[...]], axis=1)
    down = jnp.concatenate([da[...], db[...]], axis=0)
    hidden = gated(
        jnp.dot(rows, gate, preferred_element_type=jnp.float32),
        jnp.dot(rows, up, preferred_element_type=jnp.float32),
    )
    out = jnp.dot(hidden, down, preferred_element_type=jnp.float32)
    picked = [
        jnp.dot(tab[:piece_rows], ref[...], preferred_element_type=jnp.float32).astype(jnp.bfloat16)
        for tab, ref in ((own_tab, own_ref), (other_tab, other_ref))
    ]
    parts = [[], []]
    for j in range(piece_rows // cap):
        at = slice(j * cap, (j + 1) * cap)
        part = routed(jnp.concatenate([p[at] for p in picked], axis=0), j, *weights)
        parts[0].append(part[:cap])
        parts[1].append(part[cap:])
    for tab, part, half, out_ref in (
        (own_tab, parts[0], out[:tokens], own_out),
        (other_tab, parts[1], out[tokens:], other_out),
    ):
        part = jnp.concatenate(part + part, axis=0)
        share = lax.dot_general(
            tab[piece_rows:], part, (((0,), (0,)), ((), ())), preferred_element_type=jnp.float32
        )
        out_ref[...] = (half + share).astype(out_ref.dtype)


def combine_kernel(top_ref, rest_ref, shared_ref, back_ref, gain_ref, *refs):
    pieces, out_ref = refs[:-1], refs[-1]
    rows = jnp.concatenate([piece[...] for piece in pieces], axis=0)
    total = shared_ref[...] + back_ref[...].astype(jnp.float32)
    for table in (top_ref, rest_ref):
        total = total + lax.dot_general(
            table[...], rows, (((0,), (0,)), ((), ())), preferred_element_type=jnp.float32
        )
    mean_sq = jnp.mean(total * total, axis=-1, keepdims=True)
    out_ref[...] = (total * lax.rsqrt(mean_sq + EPS) * gain_ref[...]).astype(jnp.bfloat16)


def experts_near(
    moe_in,
    pre_gain,
    expert_ids,
    routed_expert_weight,
    w_gate,
    w_up,
    w_down,
    common_expert_gate_weight,
    common_expert_up_weight,
    common_expert_down_weight,
    moe_gain,
):
    tokens, width = moe_in.shape
    top_count = expert_ids.shape[1]
    local_experts, _, units = w_gate.shape
    shared_units = common_expert_gate_weight.shape[1]
    ep_size = lax.axis_size("ep")
    near_bit, far_bit = 1, lax.axis_size("tp") // 2
    experts = local_experts * ep_size
    cap = 2 * tokens * top_count // experts
    piece_rows = local_experts * cap
    own = lax.axis_index("ep")

    def array(rows, kind=jnp.bfloat16):
        return jax.ShapeDtypeStruct((rows, width), kind)

    def paired(block):
        return block, swap(block, "tp", near_bit)

    weights = (*paired(w_gate.swapaxes(1, 2)), *paired(w_up.swapaxes(1, 2)), *paired(w_down))
    common = (
        *paired(common_expert_gate_weight),
        *paired(common_expert_up_weight),
        *paired(common_expert_down_weight),
    )
    ids = expert_ids.T
    relative = ((ids // local_experts) ^ own) * local_experts + ids % local_experts
    far_rows = (ep_size - 1) * piece_rows
    table = jax.ShapeDtypeStruct((far_rows, tokens), jnp.bfloat16)
    near_table = jax.ShapeDtypeStruct((3 * piece_rows, tokens), jnp.bfloat16)
    normed, top, rest, near_tab, *pieces = run_kernel(
        functools.partial(prepare_kernel, cap),
        (array(tokens), table, table, near_table) + (array(piece_rows),) * (ep_size - 1),
        2 * ep_size * piece_rows * tokens * width,
        moe_in,
        pre_gain[None],
        relative,
        routed_expert_weight.T,
    )
    arrived = [None] + [swap(pieces[r - 1], "ep", r) for r in range(1, ep_size)]
    other_rows = swap(normed, "tp", far_bit)
    other_tab = swap(near_tab, "tp", far_bit)
    local_own, local_other = run_kernel(
        functools.partial(local_kernel, cap),
        (array(tokens, jnp.float32), array(tokens)),
        12 * width * (2 * tokens * shared_units + 2 * piece_rows * units),
        normed,
        other_rows,
        near_tab,
        other_tab,
        *common,
        *weights,
    )
    local_back = swap(local_other, "tp", far_bit)

    returned = [None] * ep_size
    for chunk in chunks_of(ep_size):
        mine = [arrived[r] for r in chunk]
        other = [swap(arrived[r], "tp", far_bit) for r in chunk]
        parts = run_kernel(
            functools.partial(routed_kernel, cap, 2 * len(chunk)),
            (array(piece_rows),) * (2 * len(chunk)),
            2 * 2 * len(chunk) * piece_rows * 3 * width * 2 * units,
            *mine,
            *other,
            *weights,
        )
        for r, part, sent in zip(chunk, parts, parts[len(chunk) :]):
            back = swap(sent, "tp", far_bit)
            total = (part.astype(jnp.float32) + back.astype(jnp.float32)).astype(jnp.bfloat16)
            returned[r] = swap(total, "ep", r)
    return run_kernel(
        combine_kernel,
        (array(tokens),),
        2 * 2 * far_rows * tokens * width,
        top,
        rest,
        local_own,
        local_back,
        moe_gain[None],
        *returned[1:],
    )[0]


def chunks_of(ep_size):
    return [list(range(1, min(4, ep_size)))] + [[r, r + 1] for r in range(4, ep_size, 2)]


def is_near(ep_size, tp_size):
    return ep_size <= NEAR_LIMIT and ep_size & (ep_size - 1) == 0 and tp_size == 4


def body(*args):
    near = is_near(lax.axis_size("ep"), lax.axis_size("tp"))
    experts_out = (experts_near if near else experts_wide)(*args[6:])
    return (attention(*args[:6]), experts_out)


def solution(mesh):
    in_specs = (
        P(("ep", "tp"), None),
        P(("ep", "tp"), None),
        P(("ep", "tp"), None),
        P(),
        P(),
        P(),
        P(("ep", "tp"), None),
        P(),
        P(("ep", "tp"), None),
        P(("ep", "tp"), None),
        P("ep", None, "tp"),
        P("ep", None, "tp"),
        P("ep", "tp", None),
        P(None, "tp"),
        P(None, "tp"),
        P("tp", None),
        P(),
    )
    out_specs = (P(("ep", "tp"), None), P(("ep", "tp"), None))
    return jax.shard_map(
        body, mesh=mesh, in_specs=in_specs, out_specs=out_specs, check_vma=False
    )
```

```python
import functools
import math

import jax
import jax.numpy as jnp
from jax import lax
from jax.experimental import pallas as pl
from jax.experimental.pallas import tpu as pltpu
from jax.sharding import PartitionSpec as P

HEADS = 16
KV_HEADS = 4
HEAD_DIM = 64
WINDOW = 128


EPS = 1e-06
NEGATIVE = -1e30
NEAR_LIMIT = 8
KERNEL_VMEM = 24 * 1024 * 1024


def from_behind(block, axis, distance):
    devices = range(lax.axis_size(axis))
    route = [(i - distance, i) for i in devices if i - distance in devices]
    return lax.ppermute(block, axis, route)


def rms_scale(inputs, gain_vec):
    mean_sq = jnp.mean(inputs * inputs, axis=-1, keepdims=True)
    return inputs * lax.rsqrt(mean_sq + EPS) * gain_vec


def slot_table(route_ids, slot_cap):
    flat_ids = route_ids.reshape(-1)
    assigned = flat_ids.shape[0]
    earlier = jnp.arange(assigned)[None, :] < jnp.arange(assigned)[:, None]
    position = jnp.sum((flat_ids[:, None] == flat_ids[None, :]) & earlier, axis=1)
    return (flat_ids * slot_cap + position).reshape(route_ids.shape)


def pack_rows(token_rows, slot_ids, slot_total):
    numbers = jnp.arange(slot_total, dtype=jnp.int32)
    chosen = jnp.any(slot_ids[None, :, :] == numbers[:, None, None], axis=2).astype(jnp.bfloat16)
    return jnp.dot(chosen, token_rows, preferred_element_type=jnp.float32).astype(jnp.bfloat16)


def attention_kernel(q_ref, k_ref, v_ref, rim_ref, sink_ref, first_ref, weight_ref, gain_ref, out_ref, mix_ref):
    lanes = 2 * HEAD_DIM
    group_size = HEADS // KV_HEADS
    blocks = q_ref.shape[0] // WINDOW
    query = lax.broadcasted_iota(jnp.int32, (WINDOW, 2 * WINDOW), 0)
    key = lax.broadcasted_iota(jnp.int32, (WINDOW, 2 * WINDOW), 1)
    inside = (key > query) & (key <= query + WINDOW)
    low = lax.broadcasted_iota(jnp.int32, (2 * WINDOW, lanes), 1) < HEAD_DIM

    def spread(tile, group):
        tile = tile.astype(jnp.float32)
        kept = jnp.where(low if group % 2 == 0 else ~low, tile, 0.0)
        moved = pltpu.roll(kept, HEAD_DIM, 1)
        both = [kept, moved] if group % 2 == 0 else [moved, kept]
        return jnp.concatenate(both, axis=0).astype(jnp.bfloat16)

    for block in range(blocks):
        at = slice(block * WINDOW, (block + 1) * WINDOW)
        before = slice((block - 1) * WINDOW, block * WINDOW)
        valid = inside
        if block == 0:
            valid = inside & (key >= first_ref[0] * WINDOW)
        for tile in range(KV_HEADS // 2):
            span = slice(tile * lanes, (tile + 1) * lanes)
            earlier_k = rim_ref[0, :, span] if block == 0 else k_ref[before, span]
            earlier_v = rim_ref[1, :, span] if block == 0 else v_ref[before, span]
            band_k = jnp.concatenate([earlier_k, k_ref[at, span]], axis=0)
            band_v = jnp.concatenate([earlier_v, v_ref[at, span]], axis=0)
            for group in (2 * tile, 2 * tile + 1):
                keys, values = spread(band_k, group), spread(band_v, group)
                for pair in range(group * group_size // 2, (group + 1) * group_size // 2):
                    cols = slice(pair * lanes, (pair + 1) * lanes)
                    scores = dot_last(q_ref[at, cols], keys) * (1.0 / math.sqrt(HEAD_DIM))
                    probs = []
                    for part in range(2):
                        sink = sink_ref[2 * pair + part]
                        own = scores[:, part * 2 * WINDOW : (part + 1) * 2 * WINDOW]
                        own = jnp.where(valid, own, NEGATIVE)
                        row_top = jnp.maximum(jnp.max(own, axis=-1, keepdims=True), sink)
                        grown = jnp.exp(own - row_top)
                        total = jnp.sum(grown, axis=-1, keepdims=True) + jnp.exp(sink - row_top)
                        probs.append((grown * (1.0 / total)).astype(jnp.bfloat16))
                    mixed = jnp.dot(
                        jnp.concatenate(probs, axis=1), values, preferred_element_type=jnp.float32
                    )
                    mix_ref[at, cols] = mixed.astype(jnp.bfloat16)
    projected = jnp.dot(mix_ref[...], weight_ref[...], preferred_element_type=jnp.float32)
    mean_sq = jnp.mean(projected * projected, axis=-1, keepdims=True)
    out_ref[...] = (projected * lax.rsqrt(mean_sq + EPS) * gain_ref[...]).astype(jnp.bfloat16)


def attention(att_queries, att_keys, att_values, sink_logits, out_weight, att_gain):
    rows, columns = att_queries.shape
    width = out_weight.shape[1]
    last = slice(rows - WINDOW, rows)
    rim = from_behind(jnp.stack([att_keys[last], att_values[last]]), ("ep", "tp"), 1)
    first = (lax.axis_index(("ep", "tp")) == 0).astype(jnp.int32)[None]
    inner, scalars = pl.BlockSpec(memory_space=pltpu.VMEM), pl.BlockSpec(memory_space=pltpu.SMEM)
    return pl.pallas_call(
        attention_kernel,
        out_shape=jax.ShapeDtypeStruct((rows, width), jnp.bfloat16),
        in_specs=[inner] * 4 + [scalars] * 2 + [inner] * 2,
        out_specs=inner,
        scratch_shapes=[pltpu.VMEM((rows, columns), jnp.bfloat16)],
        compiler_params=pltpu.CompilerParams(vmem_limit_bytes=KERNEL_VMEM),
        cost_estimate=pl.CostEstimate(
            flops=2 * rows * columns * (width + 8 * WINDOW),
            bytes_accessed=2 * (rows * columns + columns * width + rows * width),
            transcendentals=rows * HEADS * 2 * WINDOW,
        ),
    )(att_queries, att_keys, att_values, rim, sink_logits, first, out_weight, att_gain[None])


def experts_wide(
    moe_in,
    pre_gain,
    expert_ids,
    routed_expert_weight,
    w_gate,
    w_up,
    w_down,
    common_expert_gate_weight,
    common_expert_up_weight,
    common_expert_down_weight,
    moe_gain,
):
    tokens = moe_in.shape[0]
    top_count = expert_ids.shape[1]
    local_experts = w_gate.shape[0]
    ep_size = lax.axis_size("ep")
    tp_size = lax.axis_size("tp")
    experts = local_experts * ep_size
    slot_cap = 2 * tokens * top_count // experts
    slot_total = experts * slot_cap
    normed = rms_scale(moe_in.astype(jnp.float32), pre_gain).astype(jnp.bfloat16)
    own_slots = slot_table(expert_ids, slot_cap)
    packed = pack_rows(normed, own_slots, slot_total)[None]
    arrived = lax.all_to_all(packed, "ep", split_axis=1, concat_axis=1, tiled=True)
    arrived_all, tokens_all = (
        lax.all_gather(arrived[0], "tp", axis=0, tiled=True),
        lax.all_gather(normed, "tp", axis=0, tiled=True),
    )
    arrived = arrived_all.reshape(tp_size, slot_total, normed.shape[1])
    token_block = tokens_all.reshape(tp_size, tokens, normed.shape[1])
    routed = arrived
    routed = routed.reshape(
        1 * lax.axis_size("tp"), ep_size, local_experts, slot_cap, normed.shape[1]
    )
    gate_act = jnp.einsum("tsjcd,jdf->tsjcf", routed, w_gate, preferred_element_type=jnp.float32)
    up_act = jnp.einsum("tsjcd,jdf->tsjcf", routed, w_up, preferred_element_type=jnp.float32)
    hidden = (jax.nn.silu(gate_act) * up_act).astype(jnp.bfloat16)
    routed_part = jnp.einsum("tsjcf,jfd->tsjcd", hidden, w_down, preferred_element_type=jnp.float32)
    routed_part = routed_part.reshape(1 * lax.axis_size("tp"), slot_total, normed.shape[1])
    common_gate_activation = jnp.einsum(
        "spz,zv->spv", token_block, common_expert_gate_weight, preferred_element_type=jnp.float32
    )
    shared_up_act = jnp.einsum(
        "spz,zv->spv", token_block, common_expert_up_weight, preferred_element_type=jnp.float32
    )
    common_expert_hidden = (jax.nn.silu(common_gate_activation) * shared_up_act).astype(
        jnp.bfloat16
    )
    shared_part = jnp.einsum(
        "nsq,ql->nsl",
        common_expert_hidden,
        common_expert_down_weight,
        preferred_element_type=jnp.float32,
    )
    summed = lax.psum_scatter(
        jnp.concatenate([routed_part, shared_part], axis=1).astype(jnp.bfloat16),
        "tp",
        scatter_dimension=0,
        tiled=True,
    ).astype(jnp.float32)
    routed_out = summed[0, :slot_total].astype(jnp.bfloat16)
    shared_sum = summed[0, slot_total:]
    returned = lax.all_to_all(routed_out, "ep", split_axis=0, concat_axis=0, tiled=True)
    picked = returned[own_slots.reshape(-1)].reshape(tokens, top_count, normed.shape[1])
    combined = (
        jnp.sum(routed_expert_weight[:, :, None] * picked.astype(jnp.float32), axis=1) + shared_sum
    )
    experts_out = rms_scale(combined, moe_gain).astype(jnp.bfloat16)
    return experts_out


def swap(block, axis, bit):
    route = [(i, i ^ bit) for i in range(lax.axis_size(axis))]
    return lax.ppermute(block, axis, route)


def dot_last(left, right):
    return lax.dot_general(
        left, right, (((1,), (1,)), ((), ())), preferred_element_type=jnp.float32
    )


def gated(gate_act, up_act):
    return (gate_act / (1.0 + jnp.exp(-gate_act)) * up_act).astype(jnp.bfloat16)


def run_kernel(kernel, outs, flops, *operands):
    size = sum(o.size * o.dtype.itemsize for o in (*operands, *outs))
    return pl.pallas_call(
        kernel,
        out_shape=outs,
        compiler_params=pltpu.CompilerParams(vmem_limit_bytes=KERNEL_VMEM),
        cost_estimate=pl.CostEstimate(flops=flops, bytes_accessed=size, transcendentals=0),
    )(*operands)


def prepare_kernel(cap, in_ref, gain_ref, rel_ref, weight_ref, normed_ref, slot_ref, near_ref, *pieces):
    rows = in_ref[...].astype(jnp.float32)
    mean_sq = jnp.mean(rows * rows, axis=-1, keepdims=True)
    normed = (rows * lax.rsqrt(mean_sq + EPS) * gain_ref[...]).astype(jnp.bfloat16)
    normed_ref[...] = normed
    top_count, tokens = rel_ref.shape
    piece_rows = pieces[0].shape[0]
    slots = (1 + len(pieces)) * piece_rows
    experts = slots // cap
    expert_row = lax.broadcasted_iota(jnp.int32, (experts, tokens), 0)
    named = [rel_ref[k : k + 1, :] == expert_row for k in range(top_count)]
    counts = sum(jnp.where(hit, 1.0, 0.0) for hit in named)
    before = lax.broadcasted_iota(jnp.int32, (tokens, tokens), 0) < lax.broadcasted_iota(
        jnp.int32, (tokens, tokens), 1
    )
    prior = jnp.dot(
        counts.astype(jnp.bfloat16),
        jnp.where(before, 1.0, 0.0).astype(jnp.bfloat16),
        preferred_element_type=jnp.float32,
    )
    slot_row = lax.broadcasted_iota(jnp.int32, (slots, tokens), 0)
    chosen = jnp.zeros((slots, tokens), jnp.float32)
    share = jnp.zeros((piece_rows, tokens), jnp.float32)
    for k, hit in enumerate(named):
        position = jnp.sum(jnp.where(hit, prior, 0.0), axis=0, keepdims=True)
        slot = rel_ref[k : k + 1, :] * cap + position.astype(jnp.int32)
        slot_ref[k : k + 1, :] = slot
        here = slot == slot_row
        chosen = chosen + jnp.where(here, 1.0, 0.0)
        share = share + jnp.where(here[:piece_rows], weight_ref[k : k + 1, :], 0.0)
    chosen = chosen.astype(jnp.bfloat16)
    for p, piece in enumerate(pieces, 1):
        piece[...] = jnp.dot(
            chosen[p * piece_rows : (p + 1) * piece_rows],
            normed,
            preferred_element_type=jnp.float32,
        ).astype(jnp.bfloat16)
    top = share.astype(jnp.bfloat16)
    rest = (share - top.astype(jnp.float32)).astype(jnp.bfloat16)
    near_ref[...] = jnp.concatenate([chosen[:piece_rows], top, rest], axis=0)


def routed(rows, j, gate_a, gate_b, up_a, up_b, down_a, down_b):
    wide = jnp.concatenate([gate_a[j], gate_b[j], up_a[j], up_b[j]], axis=0)
    act = dot_last(rows, wide)
    half = act.shape[1] // 2
    hidden = gated(act[:, :half], act[:, half:])
    down = jnp.concatenate([down_a[j], down_b[j]], axis=0)
    return jnp.dot(hidden, down, preferred_element_type=jnp.float32).astype(jnp.bfloat16)


def routed_kernel(cap, count, *refs):
    pieces, weights, outs = refs[:count], refs[count : count + 6], refs[count + 6 :]
    for j in range(weights[0].shape[0]):
        at = slice(j * cap, (j + 1) * cap)
        rows = jnp.concatenate([piece[at, :] for piece in pieces], axis=0)
        out = routed(rows, j, *weights)
        for p, out_ref in enumerate(outs):
            out_ref[at, :] = out[p * cap : (p + 1) * cap]


def local_kernel(cap, own_ref, other_ref, own_tab, other_tab, *refs):
    ga, gb, ua, ub, da, db = refs[:6]
    weights, (own_out, other_out) = refs[6:12], refs[12:]
    tokens = own_ref.shape[0]
    piece_rows = own_tab.shape[0] // 3
    rows = jnp.concatenate([own_ref[...], other_ref[...]], axis=0)
    gate = jnp.concatenate([ga[...], gb[...]], axis=1)
    up = jnp.concatenate([ua[...], ub[...]], axis=1)
    down = jnp.concatenate([da[...], db[...]], axis=0)
    hidden = gated(
        jnp.dot(rows, gate, preferred_element_type=jnp.float32),
        jnp.dot(rows, up, preferred_element_type=jnp.float32),
    )
    out = jnp.dot(hidden, down, preferred_element_type=jnp.float32)
    picked = [
        jnp.dot(tab[:piece_rows], ref[...], preferred_element_type=jnp.float32).astype(jnp.bfloat16)
        for tab, ref in ((own_tab, own_ref), (other_tab, other_ref))
    ]
    parts = [[], []]
    for j in range(piece_rows // cap):
        at = slice(j * cap, (j + 1) * cap)
        part = routed(jnp.concatenate([p[at] for p in picked], axis=0), j, *weights)
        parts[0].append(part[:cap])
        parts[1].append(part[cap:])
    for tab, part, half, out_ref in (
        (own_tab, parts[0], out[:tokens], own_out),
        (other_tab, parts[1], out[tokens:], other_out),
    ):
        part = jnp.concatenate(part + part, axis=0)
        share = lax.dot_general(
            tab[piece_rows:], part, (((0,), (0,)), ((), ())), preferred_element_type=jnp.float32
        )
        out_ref[...] = (half + share).astype(out_ref.dtype)


def combine_kernel(slot_ref, weight_ref, shared_ref, back_ref, gain_ref, *refs):
    pieces, out_ref = refs[:-1], refs[-1]
    top_count, tokens = slot_ref.shape
    piece_rows = pieces[0].shape[0]
    far_rows = len(pieces) * piece_rows
    slot_row = lax.broadcasted_iota(jnp.int32, (far_rows, tokens), 0) + piece_rows
    share = jnp.zeros((far_rows, tokens), jnp.float32)
    for k in range(top_count):
        here = slot_ref[k : k + 1, :] == slot_row
        share = share + jnp.where(here, weight_ref[k : k + 1, :], 0.0)
    top = share.astype(jnp.bfloat16)
    rest = (share - top.astype(jnp.float32)).astype(jnp.bfloat16)
    rows = jnp.concatenate([piece[...] for piece in pieces], axis=0)
    total = shared_ref[...] + back_ref[...].astype(jnp.float32)
    for table in (top, rest):
        total = total + lax.dot_general(
            table, rows, (((0,), (0,)), ((), ())), preferred_element_type=jnp.float32
        )
    mean_sq = jnp.mean(total * total, axis=-1, keepdims=True)
    out_ref[...] = (total * lax.rsqrt(mean_sq + EPS) * gain_ref[...]).astype(jnp.bfloat16)


def experts_near(
    moe_in,
    pre_gain,
    expert_ids,
    routed_expert_weight,
    w_gate,
    w_up,
    w_down,
    common_expert_gate_weight,
    common_expert_up_weight,
    common_expert_down_weight,
    moe_gain,
):
    tokens, width = moe_in.shape
    top_count = expert_ids.shape[1]
    local_experts, _, units = w_gate.shape
    shared_units = common_expert_gate_weight.shape[1]
    ep_size = lax.axis_size("ep")
    near_bit, far_bit = 1, lax.axis_size("tp") // 2
    experts = local_experts * ep_size
    cap = 2 * tokens * top_count // experts
    piece_rows = local_experts * cap
    own = lax.axis_index("ep")

    def array(rows, kind=jnp.bfloat16):
        return jax.ShapeDtypeStruct((rows, width), kind)

    def paired(block):
        return block, swap(block, "tp", near_bit)

    weights = (*paired(w_gate.swapaxes(1, 2)), *paired(w_up.swapaxes(1, 2)), *paired(w_down))
    common = (
        *paired(common_expert_gate_weight),
        *paired(common_expert_up_weight),
        *paired(common_expert_down_weight),
    )
    ids = expert_ids.T
    relative = ((ids // local_experts) ^ own) * local_experts + ids % local_experts
    far_rows = (ep_size - 1) * piece_rows
    slot_table_shape = jax.ShapeDtypeStruct((top_count, tokens), jnp.int32)
    near_table = jax.ShapeDtypeStruct((3 * piece_rows, tokens), jnp.bfloat16)
    normed, slots, near_tab, *pieces = run_kernel(
        functools.partial(prepare_kernel, cap),
        (array(tokens), slot_table_shape, near_table) + (array(piece_rows),) * (ep_size - 1),
        2 * ep_size * piece_rows * tokens * width,
        moe_in,
        pre_gain[None],
        relative,
        routed_expert_weight.T,
    )
    arrived = [None] + [swap(pieces[r - 1], "ep", r) for r in range(1, ep_size)]
    other_rows = swap(normed, "tp", far_bit)
    other_tab = swap(near_tab, "tp", far_bit)
    local_own, local_other = run_kernel(
        functools.partial(local_kernel, cap),
        (array(tokens, jnp.float32), array(tokens)),
        12 * width * (2 * tokens * shared_units + 2 * piece_rows * units),
        normed,
        other_rows,
        near_tab,
        other_tab,
        *common,
        *weights,
    )
    local_back = swap(local_other, "tp", far_bit)

    returned = [None] * ep_size
    for chunk in chunks_of(ep_size):
        mine = [arrived[r] for r in chunk]
        other = [swap(arrived[r], "tp", far_bit) for r in chunk]
        parts = run_kernel(
            functools.partial(routed_kernel, cap, 2 * len(chunk)),
            (array(piece_rows),) * (2 * len(chunk)),
            2 * 2 * len(chunk) * piece_rows * 3 * width * 2 * units,
            *mine,
            *other,
            *weights,
        )
        for r, part, sent in zip(chunk, parts, parts[len(chunk) :]):
            back = swap(sent, "tp", far_bit)
            total = (part.astype(jnp.float32) + back.astype(jnp.float32)).astype(jnp.bfloat16)
            returned[r] = swap(total, "ep", r)
    return run_kernel(
        combine_kernel,
        (array(tokens),),
        2 * 2 * far_rows * tokens * width,
        slots,
        routed_expert_weight.T,
        local_own,
        local_back,
        moe_gain[None],
        *returned[1:],
    )[0]


def chunks_of(ep_size):
    return [list(range(1, min(4, ep_size)))] + [[r, r + 1] for r in range(4, ep_size, 2)]


def is_near(ep_size, tp_size):
    return ep_size == NEAR_LIMIT and tp_size == 4


def body(*args):
    near = is_near(lax.axis_size("ep"), lax.axis_size("tp"))
    experts_out = (experts_near if near else experts_wide)(*args[6:])
    return (attention(*args[:6]), experts_out)


def solution(mesh):
    in_specs = (
        P(("ep", "tp"), None),
        P(("ep", "tp"), None),
        P(("ep", "tp"), None),
        P(),
        P(),
        P(),
        P(("ep", "tp"), None),
        P(),
        P(("ep", "tp"), None),
        P(("ep", "tp"), None),
        P("ep", None, "tp"),
        P("ep", None, "tp"),
        P("ep", "tp", None),
        P(None, "tp"),
        P(None, "tp"),
        P("tp", None),
        P(),
    )
    out_specs = (P(("ep", "tp"), None), P(("ep", "tp"), None))
    return jax.shard_map(
        body, mesh=mesh, in_specs=in_specs, out_specs=out_specs, check_vma=False
    )
```
